32 devices in a mesh: ep: 8 (over z, x), tp: 4 (over y, core).
Axes of the slice: x: 2, y: 2, z: 4, core: 2. Of those that a mesh axis runs over, the one named last changes fastest.
Arguments:
- tokens: bfloat16 [1024, 2048], P('ep', 'tp'), may hold values from -6 to 6
- cotangent: bfloat16 [1024, 2048], P('ep', 'tp'), may hold values from -6 to 6
- experts: int32 [1024, 2], P('ep'), may hold values from 0 to 7, as said below
- combine: float32 [1024, 2], P('ep'), may hold values from 0.2 to 1
- w_gate: bfloat16 [8, 2048, 256], P('ep', 'tp'), may hold values from -0.125 to 0.125
- w_up: bfloat16 [8, 2048, 256], P('ep', 'tp'), may hold values from -0.125 to 0.125
- w_down: bfloat16 [8, 256, 2048], P('ep', None, 'tp'), may hold values from -0.375 to 0.375
Outputs:
- grad_tokens: bfloat16 [1024, 2048], P('ep', 'tp')
- grad_combine: float32 [1024, 2], P('ep')
- gate_grad: float32 [8, 2048, 256], P('ep', 'tp')
- up_grad: float32 [8, 2048, 256], P('ep', 'tp')
- down_grad: float32 [8, 256, 2048], P('ep', None, 'tp')
The draws below stay inside these ranges and needn't reach their ends.
Inputs may be any that keep to these rules, and one draw needn't show every extreme that they name: Each row names two different experts of one group of 4 consecutive experts. The rows of one index of ep name any one expert at most 64 times, and some expert exactly 64 times.
All inputs are finite; a program needn't handle non-finite values.
Results may differ from the reference program's by a relative error of at most 0.019.
Values may be sent and summed in bfloat16 or wider, within the bound.
No kernel may reach another device: no remote copies, remote signals or barrier semaphores. Data moves between devices by JAX's collectives and lax.ppermute only.
A program may use at most 64 MiB of HBM per device.

```python
import jax
import jax.numpy as jnp
from jax import lax

D = 2048
FE = 256
TOPK = 2
GSIZE = 4
TOK_DEV = 128
TOKENS = 1024
EXPERTS = 8
GROUPS = 2
CAP = 64
N_EP = 8
N_TP = 4


def draw_experts(key, part):
    base_group = jax.random.randint(jax.random.fold_in(key, 7), (), 0, GROUPS).astype(jnp.int32)
    device_keys = jax.random.split(jax.random.fold_in(key, 11), N_EP)
    device_ids = jnp.arange(N_EP, dtype=jnp.int32)

    def one_device(device_key, device_id):
        keys_four = jax.random.split(device_key, 4)
        hot_group = ((base_group + device_id) % GROUPS).astype(jnp.int32)
        pair_count = GROUPS // 2
        step_range = CAP // 4
        shifts = 4 * jax.random.randint(keys_four[0], (pair_count,), -step_range, step_range + 1).astype(jnp.int32)
        shifts = shifts.at[0].set(CAP)
        quotas = jnp.stack([CAP + shifts, CAP - shifts], axis=1).reshape(GROUPS).astype(jnp.int32)
        others = (hot_group + 1 + jnp.arange(GROUPS - 1, dtype=jnp.int32)) % GROUPS
        placed = jnp.concatenate([hot_group[None], jax.random.permutation(keys_four[1], others).astype(jnp.int32)])
        bounds = jnp.cumsum(quotas).astype(jnp.int32)
        ranks = jnp.arange(TOK_DEV, dtype=jnp.int32)
        position = jnp.searchsorted(bounds, ranks, side='right').astype(jnp.int32)
        within = ranks - (bounds[position] - quotas[position])
        inner_keys = jax.random.split(keys_four[2], GROUPS)
        inner_order = jax.vmap(lambda inner_key: jax.random.permutation(inner_key, GSIZE))(inner_keys).astype(jnp.int32)
        first_pick = inner_order[position, within % GSIZE]
        second_pick = inner_order[position, (within + 1) % GSIZE]
        expert_ids = placed[position][:, None] * GSIZE + jnp.stack([first_pick, second_pick], axis=1)
        order = jax.random.permutation(keys_four[3], TOK_DEV)
        return expert_ids[order].astype(jnp.int32)
    return jax.vmap(one_device)(device_keys, device_ids).reshape(TOKENS, TOPK)


def shard_levels(stream_key, extent, shards, least, top_value):
    def one(dim, parts):
        heights = jax.random.uniform(jax.random.fold_in(jax.random.fold_in(stream_key, 6), dim), (parts,), jnp.float32, least / len(shards), top_value / len(shards))
        return jnp.repeat(jnp.exp(heights), extent[dim] // parts).reshape((-1,) + (1,) * (len(extent) - dim - 1))

    factor_of = one(*shards[0])
    for cut in shards[1:]:
        factor_of = factor_of * one(*cut)
    return factor_of


def normal_values(stream_key, extent, deviation, bound, shards=(), held_as=jnp.bfloat16):
    gain = shard_levels(stream_key, extent, shards, -0.22, 0.18) if shards else 1.0
    result = jax.random.normal(stream_key, extent, jnp.float32) * deviation * gain
    return jnp.minimum(jnp.maximum(result, -bound), bound).astype(held_as)


def setup_inputs(seed: int = 0) -> dict:
    key_list = jax.random.split(jax.random.key(seed), 8)
    tokens = normal_values(key_list[0], (TOKENS, D), 1.0, 6.0, ((0, 8), (1, 4)))
    cotangent = normal_values(key_list[1], (TOKENS, D), 1.0, 6.0, ((0, 8), (1, 4)))
    experts = draw_experts(jax.random.fold_in(key_list[7], 71), 0)
    combine = jnp.clip(0.2 + 0.8 * jax.random.uniform(key_list[3], (TOKENS, TOPK), jnp.float32) ** shard_levels(key_list[3], (TOKENS, TOPK), ((0, 8),), -0.2, 0.2), 0.2, 1.0)
    w_gate = normal_values(key_list[4], (EXPERTS, D, FE), D ** -0.5, 0.125, ((0, 8), (1, 4)))
    w_up = normal_values(key_list[5], (EXPERTS, D, FE), D ** -0.5, 0.125, ((0, 8), (1, 4)))
    w_down = normal_values(key_list[6], (EXPERTS, FE, D), FE ** -0.5, 0.375, ((0, 8), (2, 4)))
    return dict(tokens=tokens, cotangent=cotangent, experts=experts, combine=combine, w_gate=w_gate, w_up=w_up, w_down=w_down)


def slot_table(experts):
    routed = experts.reshape(N_EP, TOK_DEV * TOPK).astype(jnp.int32)
    onehot = (routed[:, :, None] == jnp.arange(EXPERTS, dtype=jnp.int32)[None, None, :]).astype(jnp.int32)
    earlier = jnp.sum((jnp.cumsum(onehot, axis=1) - onehot) * onehot, axis=2).astype(jnp.int32)
    position = jnp.arange(N_EP, dtype=jnp.int32)[:, None] * CAP + earlier
    assigned = jnp.arange(TOKENS * TOPK, dtype=jnp.int32).reshape(N_EP, TOK_DEV * TOPK)
    table = jnp.full((EXPERTS, N_EP * CAP), -1, jnp.int32)
    return table.at[routed, position].set(assigned)


def block_sum(partial_sum):
    rounded = lax.optimization_barrier(partial_sum.astype(jnp.bfloat16)).astype(jnp.float32)
    return jnp.sum(rounded, axis=1)


def reference(tokens, cotangent, experts, combine, w_gate, w_up, w_down):
    table = slot_table(experts)
    weight_flat = lax.optimization_barrier(combine.astype(jnp.bfloat16)).astype(jnp.float32).reshape(-1)
    width_block = D // N_TP
    highest = lax.Precision.HIGHEST

    def per_expert(running, inputs):
        grad_acc, comb_acc = running
        row_ids, gate_mat, up_mat, down_mat = inputs
        filled = row_ids >= 0
        source = jnp.maximum(row_ids, 0)
        token_ids = (source // TOPK).astype(jnp.int32)
        filled_col = filled[:, None]
        rows = jnp.where(filled_col, tokens[token_ids], jnp.zeros((), jnp.bfloat16))
        cots = jnp.where(filled_col, cotangent[token_ids], jnp.zeros((), jnp.bfloat16))
        weights = jnp.where(filled, weight_flat[source], jnp.float32(0.0))[:, None]
        rows_split = rows.astype(jnp.float32).reshape(-1, N_TP, width_block)
        cots_split = cots.astype(jnp.float32).reshape(-1, N_TP, width_block)
        gate_blocks = gate_mat.astype(jnp.float32).reshape(N_TP, width_block, FE)
        up_blocks = up_mat.astype(jnp.float32).reshape(N_TP, width_block, FE)
        down_blocks = down_mat.astype(jnp.float32).reshape(FE, N_TP, width_block)
        gate_pre = block_sum(jnp.einsum('rjd,jdf->rjf', rows_split, gate_blocks, precision=highest))
        up_pre = block_sum(jnp.einsum('rjd,jdf->rjf', rows_split, up_blocks, precision=highest))
        grad_scaled = block_sum(jnp.einsum('rjd,fjd->rjf', cots_split, down_blocks, precision=highest))
        sigmoid_val = jax.nn.sigmoid(gate_pre)
        silu_val = gate_pre * sigmoid_val
        hidden = silu_val * up_pre
        scaled = (weights * hidden).astype(jnp.bfloat16)
        comb_part = jnp.sum(hidden * grad_scaled, axis=1)
        grad_hidden = weights * grad_scaled
        grad_gate_pre = (grad_hidden * up_pre * sigmoid_val * (1.0 + gate_pre * (1.0 - sigmoid_val))).astype(jnp.bfloat16)
        grad_up_pre = (grad_hidden * silu_val).astype(jnp.bfloat16)
        down_grad = jnp.dot(scaled.T, cots, preferred_element_type=jnp.float32)
        gate_grad = jnp.dot(rows.T, grad_gate_pre, preferred_element_type=jnp.float32)
        up_grad = jnp.dot(rows.T, grad_up_pre, preferred_element_type=jnp.float32)
        slot_grad = (jnp.dot(grad_gate_pre, gate_mat.T, preferred_element_type=jnp.float32) + jnp.dot(grad_up_pre, up_mat.T, preferred_element_type=jnp.float32)).astype(jnp.bfloat16)
        grad_acc = grad_acc.at[token_ids].add(jnp.where(filled_col, slot_grad.astype(jnp.float32), jnp.float32(0.0)))
        comb_acc = comb_acc.at[source].add(jnp.where(filled, comb_part, jnp.float32(0.0)))
        return (grad_acc, comb_acc), (gate_grad, up_grad, down_grad)

    start_carry = (jnp.zeros((TOKENS, D), jnp.float32), jnp.zeros((TOKENS * TOPK,), jnp.float32))
    (grad_acc, comb_acc), (gate_grad, up_grad, down_grad) = lax.scan(per_expert, start_carry, (table, w_gate, w_up, w_down))
    return grad_acc.astype(jnp.bfloat16), comb_acc.reshape(TOKENS, TOPK), gate_grad, up_grad, down_grad
```

```python
import functools

import jax
import jax.numpy as jnp
from jax import lax
from jax.experimental import pallas as pl
from jax.experimental.pallas import tpu as pltpu
from jax.sharding import PartitionSpec as P

BF = jnp.bfloat16
F32 = jnp.float32
VM = pl.BlockSpec(memory_space=pltpu.VMEM)
NT = (((1,), (1,)), ((), ()))
TN = (((0,), (0,)), ((), ()))
PAD = 8


def dot(a, b, dims=(((1,), (0,)), ((), ()))):
    return lax.dot_general(a, b, dims, preferred_element_type=F32)


def call(kernel, outs, name, *args, flops=1 << 20):
    return pl.pallas_call(
        kernel,
        out_shape=[jax.ShapeDtypeStruct(s, d) for s, d in outs],
        in_specs=[VM] * len(args),
        out_specs=[VM] * len(outs),
        name=name,
        cost_estimate=pl.CostEstimate(flops=flops, bytes_accessed=1 << 20, transcendentals=0),
    )(*args)


def prep_kernel(cap, peers, e_ref, c_ref, tok_ref, cot_ref, g_ref, w_ref, *bufs):
    me = lax.axis_index("ep")
    tokens = tok_ref.shape[0]
    ids = lax.broadcasted_iota(jnp.int32, (peers, tokens), 0) ^ me
    first, second = e_ref[0:1, :] == ids, e_ref[1:2, :] == ids
    used = first | second
    weight = jnp.where(first, c_ref[0:1, :], 0.0) + jnp.where(second, c_ref[1:2, :], 0.0)
    weight = weight.astype(BF)
    w_ref[...] = weight.astype(F32)
    row = lax.broadcasted_iota(jnp.int32, (tokens, tokens), 0)
    col = lax.broadcasted_iota(jnp.int32, (tokens, tokens), 1)
    before = jnp.where(row < col, 1.0, 0.0).astype(BF)
    place = dot(jnp.where(used, 1.0, 0.0).astype(BF), before)
    place = jnp.where(used, place, -1.0)
    slot = lax.broadcasted_iota(jnp.int32, (cap, tokens), 0).astype(F32)
    for k in range(peers):
        hit = place[k : k + 1, :] == slot
        pick = jnp.where(hit, 1.0, 0.0).astype(BF)
        scaled = jnp.where(hit, weight[k : k + 1, :].astype(F32), 0.0).astype(BF)
        g_ref[k * cap : (k + 1) * cap, :] = pick
        bufs[k][0:cap, :] = dot(pick, tok_ref[...]).astype(BF)
        bufs[k][cap : 2 * cap, :] = dot(scaled, cot_ref[...]).astype(BF)


def parts_kernel(cap, n, wg_ref, wu_ref, wd_ref, *refs):
    bufs, (keep_ref, send_ref) = refs[:n], refs[n:]
    low = (lax.axis_index("tp") & 1) == 0
    fe = wg_ref.shape[1]
    half = n // 2 * cap
    rows = jnp.concatenate([b[0:cap, :] for b in bufs], axis=0)
    cots = jnp.concatenate([b[cap : 2 * cap, :] for b in bufs], axis=0)
    for i, part in enumerate(
        (dot(rows, wg_ref[...]), dot(rows, wu_ref[...]), dot(cots, wd_ref[...], NT))
    ):
        part = part.astype(BF)
        a, b = part[:half], part[half:]
        keep_ref[:, i * fe : (i + 1) * fe] = jnp.where(low, a, b)
        send_ref[:, i * fe : (i + 1) * fe] = jnp.where(low, b, a)


def act_kernel(cap, n, own_ref, far_ref, out_ref):
    half = n // 2 * cap
    fe = own_ref.shape[1] // 3
    total = own_ref[...].astype(F32) + far_ref[...].astype(F32)
    gate, up, back = total[:, :fe], total[:, fe : 2 * fe], total[:, 2 * fe :]
    sig = jax.nn.sigmoid(gate)
    silu = gate * sig
    hidden = silu * up
    comb = jnp.sum(hidden * back, axis=1, keepdims=True)
    out_ref[0:half, 0:fe] = hidden.astype(BF)
    out_ref[0:half, fe : 2 * fe] = (back * up * sig * (1.0 + gate * (1.0 - sig))).astype(BF)
    out_ref[0:half, 2 * fe :] = (back * silu).astype(BF)
    eye = lax.broadcasted_iota(jnp.int32, (cap, 128), 0) == lax.broadcasted_iota(
        jnp.int32, (cap, 128), 1
    )
    line = lax.broadcasted_iota(jnp.int32, (PAD, 128), 0)
    tail = jnp.zeros((PAD, 128), F32)
    for i in range(n // 2):
        flat = jnp.sum(jnp.where(eye, comb[i * cap : (i + 1) * cap], 0.0), axis=0, keepdims=True)
        high = flat.astype(BF).astype(F32)
        tail = tail + jnp.where(line == 2 * i, high, 0.0)
        tail = tail + jnp.where(line == 2 * i + 1, flat - high, 0.0)
    out_ref[half : half + PAD, :] = jnp.zeros((PAD, 3 * fe), BF)
    out_ref[half : half + PAD, 0:128] = tail.astype(BF)


def back_kernel(cap, n, wg_ref, wu_ref, own_ref, far_ref, act_ref, *rets):
    low = (lax.axis_index("tp") & 1) == 0
    half = n // 2 * cap
    fe = wg_ref.shape[1]
    own, far = own_ref[...], far_ref[...]
    a, b = jnp.where(low, own, far), jnp.where(low, far, own)
    act_ref[0:half, :] = a[0:half]
    act_ref[half : 2 * half, :] = b[0:half]
    act = act_ref[...]
    grad = dot(act[:, fe : 2 * fe], wg_ref[...], NT) + dot(act[:, 2 * fe :], wu_ref[...], NT)
    grad = grad.astype(BF)
    line = lax.broadcasted_iota(jnp.int32, (PAD, 128), 0)
    for i in range(n):
        tail = (a, b)[i // (n // 2)][half : half + PAD, 0:128].astype(F32)
        j = 2 * (i % (n // 2))
        tail = jnp.where(line == 0, tail[j : j + 1], 0.0) + jnp.where(
            line == 1, tail[j + 1 : j + 2], 0.0
        )
        rets[i][0:cap, :] = grad[i * cap : (i + 1) * cap]
        rets[i][cap : cap + PAD, :] = jnp.zeros((PAD, rets[i].shape[1]), BF)
        rets[i][cap : cap + PAD, 0:128] = tail.astype(BF)


def weight_kernel(cap, n_bufs, n_acts, *refs):
    bufs, acts = refs[:n_bufs], refs[n_bufs : n_bufs + n_acts]
    gate_ref, up_ref, down_ref = refs[n_bufs + n_acts :]
    fe = gate_ref.shape[1]
    rows = jnp.concatenate([b[0:cap, :] for b in bufs], axis=0)
    cots = jnp.concatenate([b[cap : 2 * cap, :] for b in bufs], axis=0)
    act = jnp.concatenate([a[...] for a in acts], axis=0)
    gate_ref[...] = dot(rows, act[:, fe : 2 * fe], TN)
    up_ref[...] = dot(rows, act[:, 2 * fe :], TN)
    down_ref[...] = dot(act[:, :fe], cots, TN)


def combine_kernel(cap, peers, e_ref, w_ref, g_ref, *refs):
    rets, (tok_ref, comb_ref) = refs[:peers], refs[peers:]
    me = lax.axis_index("ep")
    grads = jnp.concatenate([r[0:cap, :] for r in rets], axis=0)
    tok_ref[...] = dot(g_ref[...], grads, TN).astype(BF)
    first = jnp.zeros((1, e_ref.shape[1]), F32)
    second = first
    for k in range(peers):
        both = dot(rets[k][cap : cap + PAD, 0:cap], g_ref[k * cap : (k + 1) * cap, :])
        weight = w_ref[k : k + 1, :]
        value = (both[0:1] + both[1:2]) / jnp.where(weight > 0.0, weight, 1.0)
        first = jnp.where(e_ref[0:1, :] == (me ^ k), value, first)
        second = jnp.where(e_ref[1:2, :] == (me ^ k), value, second)
    comb_ref[0:1, :] = first
    comb_ref[1:2, :] = second


def chunks_of(peers):
    near = list(range(peers // 2))
    far = list(range(peers // 2, peers))
    return [near] + [far[i : i + 2] for i in range(0, len(far), 2)]


def body(tokens, cotangent, experts, combine, w_gate, w_up, w_down):
    peers = lax.axis_size("ep")
    tp = lax.axis_size("tp")
    tok_count, width = tokens.shape
    picks = experts.shape[1]
    cap = 2 * tok_count * picks // peers
    fe = w_gate.shape[2]
    wg, wu, wd = w_gate[0], w_up[0], w_down[0]

    def swap_ep(x, k):
        return lax.ppermute(x, "ep", [(i, i ^ k) for i in range(peers)])

    def swap_tp(x, k):
        return lax.ppermute(x, "tp", [(i, i ^ k) for i in range(tp)])

    e2, c2 = experts.T, combine.T
    pick, weight, *bufs = call(
        functools.partial(prep_kernel, cap, peers),
        [((peers * cap, tok_count), BF), ((peers, tok_count), F32)]
        + [((2 * cap, width), BF)] * peers,
        "prep",
        e2,
        c2,
        tokens,
        cotangent,
    )
    chunks = chunks_of(peers)
    send_order = [k for c in chunks[1:] + chunks[:1] for k in c if k]
    got = {0: bufs[0]}
    for k in send_order:
        got[k] = swap_ep(bufs[k], k)
    acts, rets = [], {}
    for ks in chunks:
        n = len(ks)
        half = n // 2 * cap
        mine = [got[k] for k in ks]
        keep, send = call(
            functools.partial(parts_kernel, cap, n),
            [((half, 3 * fe), BF)] * 2,
            "parts",
            wg,
            wu,
            wd,
            *mine,
        )
        near = swap_tp(send, 1)
        pair = (keep.astype(F32) + near.astype(F32)).astype(BF)
        far = swap_tp(pair, 2)
        (out,) = call(
            functools.partial(act_kernel, cap, n), [((half + PAD, 3 * fe), BF)], "act", pair, far
        )
        other = swap_tp(out, 1)
        act, *back = call(
            functools.partial(back_kernel, cap, n),
            [((2 * half, 3 * fe), BF)] + [((cap + PAD, width), BF)] * n,
            "back",
            wg,
            wu,
            out,
            other,
        )
        acts.append(act)
        for k, r in zip(ks, back):
            rets[k] = swap_ep(r, k) if k else r
    order = [k for c in chunks for k in c]
    gate_grad, up_grad, down_grad = call(
        functools.partial(weight_kernel, cap, peers, len(acts)),
        [((width, fe), F32), ((width, fe), F32), ((fe, width), F32)],
        "weights",
        *[got[k] for k in order],
        *acts,
    )
    grad_tokens, comb = call(
        functools.partial(combine_kernel, cap, peers),
        [((tok_count, width), BF), ((picks, tok_count), F32)],
        "combine",
        e2,
        weight,
        pick,
        *[rets[k] for k in range(peers)],
    )
    return grad_tokens, comb.T, gate_grad[None], up_grad[None], down_grad[None]


def slot_positions(routed, total_experts, capacity):
    onehot = (routed[:, None] == jnp.arange(total_experts, dtype=jnp.int32)[None, :]).astype(
        jnp.int32
    )
    earlier = jnp.sum((jnp.cumsum(onehot, axis=0) - onehot) * onehot, axis=1)
    return routed * capacity + earlier


def activation(gate_pre, up_pre, grad_scaled, weight_grid):
    sigmoid_val = jax.nn.sigmoid(gate_pre)
    silu_val = gate_pre * sigmoid_val
    hidden = silu_val * up_pre
    scaled = (weight_grid * hidden).astype(jnp.bfloat16)
    comb_part = jnp.sum(hidden * grad_scaled, axis=3)
    grad_hidden = weight_grid * grad_scaled
    grad_gate_pre = (
        grad_hidden * up_pre * sigmoid_val * (1.0 + gate_pre * (1.0 - sigmoid_val))
    ).astype(jnp.bfloat16)
    grad_up_pre = (grad_hidden * silu_val).astype(jnp.bfloat16)
    return (scaled, grad_gate_pre, grad_up_pre, comb_part)


def general_body(tokens, cotangent, experts, combine, w_gate, w_up, w_down):
    peers = lax.axis_size("ep")
    local_experts = w_gate.shape[0]
    total_experts = local_experts * peers
    tok_count = tokens.shape[0]
    picks = experts.shape[1]
    assigns = tok_count * picks
    capacity = 2 * assigns // total_experts
    per_peer = local_experts * capacity
    block_width = tokens.shape[1]
    slot_index = slot_positions(experts.reshape(assigns), total_experts, capacity)
    slot_owner = (
        jnp.zeros((total_experts * capacity,), jnp.int32)
        .at[slot_index]
        .set(jnp.arange(assigns, dtype=jnp.int32) + 1)
    )
    filled = slot_owner > 0
    source = jnp.maximum(slot_owner - 1, 0)
    token_ids = source // picks
    filled_col = filled[:, None]
    send_rows = jnp.where(
        filled_col, jnp.take(tokens, token_ids, axis=0), jnp.zeros((), jnp.bfloat16)
    ).reshape(peers, per_peer, block_width)
    send_cots = jnp.where(
        filled_col, jnp.take(cotangent, token_ids, axis=0), jnp.zeros((), jnp.bfloat16)
    ).reshape(peers, per_peer, block_width)
    send_weights = (
        jnp.where(filled, jnp.take(combine.reshape(assigns), source), jnp.float32(0.0))
        .astype(jnp.bfloat16)
        .reshape(peers, per_peer)
    )
    exchange = functools.partial(
        lax.all_to_all, axis_name="ep", split_axis=0, concat_axis=0, tiled=True
    )
    recv_rows, recv_cots, recv_weights = (
        exchange(send_rows),
        exchange(send_cots),
        exchange(send_weights),
    )
    rows_grid = recv_rows.reshape(peers, local_experts, capacity, block_width)
    cots_grid = recv_cots.reshape(peers, local_experts, capacity, block_width)
    weight_grid = recv_weights.astype(jnp.float32).reshape(peers, local_experts, capacity, 1)
    gate_part = jnp.einsum(
        "secd,edf->secf", rows_grid, w_gate, preferred_element_type=jnp.float32
    ).astype(jnp.bfloat16)
    up_part = jnp.einsum(
        "secd,edf->secf", rows_grid, w_up, preferred_element_type=jnp.float32
    ).astype(jnp.bfloat16)
    down_part = jnp.einsum(
        "secd,efd->secf", cots_grid, w_down, preferred_element_type=jnp.float32
    ).astype(jnp.bfloat16)
    gate_pre, up_pre, grad_scaled = (
        lax.psum(gate_part, "tp").astype(jnp.float32),
        lax.psum(up_part, "tp").astype(jnp.float32),
        lax.psum(down_part, "tp").astype(jnp.float32),
    )
    scaled, grad_gate_pre, grad_up_pre, comb_part = activation(
        gate_pre, up_pre, grad_scaled, weight_grid
    )
    down_grad = jnp.einsum("secf,secd->efd", scaled, cots_grid, preferred_element_type=jnp.float32)
    gate_grad = jnp.einsum(
        "secd,secf->edf", rows_grid, grad_gate_pre, preferred_element_type=jnp.float32
    )
    up_grad = jnp.einsum(
        "secd,secf->edf", rows_grid, grad_up_pre, preferred_element_type=jnp.float32
    )
    slot_sum = jnp.einsum(
        "secf,edf->secd", grad_gate_pre, w_gate, preferred_element_type=jnp.float32
    )
    slot_sum = slot_sum + jnp.einsum(
        "secf,edf->secd", grad_up_pre, w_up, preferred_element_type=jnp.float32
    )
    slot_grad = slot_sum.astype(jnp.bfloat16).reshape(peers, per_peer, block_width)
    full_grad = exchange(slot_grad).reshape(total_experts * capacity, block_width)
    comb_back = exchange(comb_part.reshape(peers, per_peer))
    per_assign = (
        jnp.take(full_grad, slot_index, axis=0)
        .astype(jnp.float32)
        .reshape(tok_count, picks, block_width)
    )
    grad_tokens = jnp.sum(per_assign, axis=1).astype(jnp.bfloat16)
    grad_combine = jnp.take(comb_back.reshape(total_experts * capacity), slot_index).reshape(
        tok_count, picks
    )
    return (grad_tokens, grad_combine, gate_grad, up_grad, down_grad)


def pick_body(tokens, cotangent, experts, combine, w_gate, w_up, w_down):
    peers, tp = lax.axis_size("ep"), lax.axis_size("tp")
    cap = 2 * tokens.shape[0] * experts.shape[1] // peers
    fits = (
        w_gate.shape[0] == 1
        and experts.shape[1] == 2
        and peers == 8
        and tp == 4
        and cap % 16 == 0
        and cap <= 128
        and tokens.shape[0] % 128 == 0
        and tokens.shape[1] % 128 == 0
        and w_gate.shape[2] % 128 == 0
    )
    chosen = body if fits else general_body
    return chosen(tokens, cotangent, experts, combine, w_gate, w_up, w_down)


def solution(mesh):
    return jax.shard_map(
        pick_body,
        mesh=mesh,
        in_specs=(
            P("ep", "tp"),
            P("ep", "tp"),
            P("ep", None),
            P("ep", None),
            P("ep", "tp", None),
            P("ep", "tp", None),
            P("ep", None, "tp"),
        ),
        out_specs=(
            P("ep", "tp"),
            P("ep", None),
            P("ep", "tp", None),
            P("ep", "tp", None),
            P("ep", None, "tp"),
        ),
        check_vma=False,
    )
```
